1024 devices in a mesh: ep: 32 (over z, core), tp: 32 (over y, x).
Axes of the slice: x: 4, y: 8, z: 16, core: 2. Of those that a mesh axis runs over, the one named last changes fastest.
Arguments:
- tokens: bfloat16 [6144, 4096], P('ep'), may hold values from -6 to 6
- expert_ids: int32 [6144, 2], P('ep'), may hold values from 0 to 31, all different within a row; in each aligned block of 192 rows (0 to 191, 192 to 383, ...) at most 15 rows name the same one
- route_weight: float32 [6144, 2], P('ep'), may hold values from 0.1 to 1
- norm_gain: float32 [4096], replicated, may hold values from 0.1 to 1.9
- gate_weight: bfloat16 [32, 4096, 4096], P('ep', None, 'tp'), may hold values from -0.28125 to 0.28125
- up_weight: bfloat16 [32, 4096, 4096], P('ep', None, 'tp'), may hold values from -0.28125 to 0.28125
- down_weight: bfloat16 [32, 4096, 4096], P('ep', None, 'tp'), may hold values from -0.028076172 to 0.028076172
Outputs:
- mixed: bfloat16 [6144, 4096], P('ep', 'tp')
The draws below stay inside these ranges and needn't reach their ends.
Inputs may be any that keep to these rules, and one draw needn't show every extreme that they name: `expert_ids`: each row names 2 different experts. In each aligned block of 192 rows (the tokens of one index of ep) no expert is named by more than 15 rows, and in some block some expert is named by exactly 15 rows.
All inputs are finite; a program needn't handle non-finite values.
Results may differ from the reference program's by a relative error of at most 0.007.
Values may be sent and summed in bfloat16 or wider, within the bound.
No kernel may reach another device: no remote copies, remote signals or barrier semaphores. Data moves between devices by JAX's collectives and lax.ppermute only.
A program may use at most 32 MiB of HBM per device.

```python
import math
import jax
import jax.numpy as jnp
import numpy as np
from jax import lax

D = 4096
FF = 4096
TOPK = 2
TOK_EP = 192
EXPERTS = 32
TOKENS = 6144
CAP = 15
N_EP = 32


def block_scale(key, extent, pieces, least, top_value):
    level, own = 1.0, jax.random.fold_in(key, 6)
    for axis_at, parts in pieces:
        draws = jnp.exp(jax.random.uniform(jax.random.fold_in(own, axis_at), (parts,), jnp.float32, least / len(pieces), top_value / len(pieces)))
        level = level * jnp.repeat(draws, extent[axis_at] // parts).reshape([-1 if axis == axis_at else 1 for axis in range(len(extent))])
    return level


def shared_out(stream_key, own, number, rows, number_of, top, bound, skew):
    ranking = jax.random.permutation(stream_key, number_of)
    heavy_load, usual = load_shares(number_of, rows * top, bound, skew, True), load_shares(number_of, rows * top, bound, skew, False)
    places = jnp.arange(number_of)

    def named(lengths, turn):
        used = int((lengths > 0).sum())
        fixed = max(1, used // 4)
        shifted = fixed + (places - fixed + turn * (used - fixed)) % max(1, number_of - fixed)
        return jnp.zeros((number_of,), jnp.int32).at[ranking[jnp.where(places < fixed, places, shifted)]].set(jnp.asarray(lengths, jnp.int32))

    lengths = jnp.where(number % 4 == 0, named(heavy_load, number // 4), named(usual, number - number // 4 - 1))
    mixed = jax.random.permutation(jax.random.fold_in(own, 3), number_of)
    source_of, receiver = mixed[0:number_of // 2 * 2:2], mixed[1:number_of // 2 * 2:2]
    margin = jnp.minimum(lengths[source_of] - 1, bound - lengths[receiver]) // 2
    margin = jnp.where((source_of == ranking[0]) | (receiver == ranking[0]) | (lengths[receiver] == 0), 0, jnp.maximum(margin, 0))
    shifted = jax.random.randint(jax.random.fold_in(own, 4), (number_of // 2,), 0, 1 << 20) % (margin + 1)
    lengths = lengths.at[source_of].add(-shifted).at[receiver].add(shifted)
    items = jnp.searchsorted(jnp.cumsum(lengths), jnp.arange(rows * top), side="right").astype(jnp.int32)
    listing = items.reshape(top, rows).T
    listing = listing[jax.random.permutation(jax.random.fold_in(own, 1), rows)]
    turn = jax.random.randint(jax.random.fold_in(own, 2), (rows, 1), 0, top)
    return jnp.take_along_axis(listing, (jnp.arange(top)[None, :] + turn) % top, axis=1)


def load_shares(count, total, bound, slope, full):
    weights = [(1 << 20) // math.isqrt(standing ** slope) + 1 for standing in range(1, count + 1)]
    largest = bound if full else min(bound, max(-(-total // count), total * weights[0] // sum(weights)))
    least = 1 if total - largest >= count - 1 else 0
    counts, rest = [largest] + [least] * (count - 1), total - largest - least * (count - 1)
    while rest > 0:
        candidates = [i for i in range(1, count) if counts[i] < largest] or [i for i in range(1, count) if counts[i] < bound]
        whole, left = sum([weights[i] for i in candidates]), rest
        for i in candidates:
            extra = min(bound - counts[i], max(1, left * weights[i] // whole), rest)
            counts[i] = counts[i] + extra
            rest = rest - extra
    return np.array(counts)


def scatter_about(stream_key, dims, deviation, bound, cuts=(), kind=jnp.bfloat16):
    gain = block_scale(stream_key, dims, cuts, -0.22, 0.18) if cuts else 1.0
    entries = jax.random.normal(stream_key, dims, jnp.float32) * deviation * gain
    return jnp.minimum(jnp.maximum(entries, -bound), bound).astype(kind)


def setup_inputs(seed: int = 0) -> dict:
    keys = jax.random.split(jax.random.key(seed), 8)
    tokens = scatter_about(keys[0], (TOKENS, D), 1.0, 6.0, ((0, 32),))
    expert_ids_keys = jax.random.split(jax.random.fold_in(keys[1], 1), TOKENS // TOK_EP)
    expert_ids_turns = jax.random.permutation(jax.random.fold_in(keys[1], 3), TOKENS // TOK_EP)
    expert_ids = jax.vmap(lambda own, number: shared_out(jax.random.fold_in(keys[1], 2), own, number, TOK_EP, EXPERTS, TOPK, CAP, 2))(expert_ids_keys, expert_ids_turns).reshape((TOKENS, TOPK))
    route_weight = jnp.clip(0.1 + 0.9 * jax.random.uniform(keys[2], (TOKENS, TOPK), jnp.float32) ** block_scale(keys[2], (TOKENS, TOPK), ((0, 32),), -0.2, 0.2), 0.1, 1.0)
    norm_gain = jnp.clip(1.0 + 0.18 * jax.random.normal(keys[3], (D,), jnp.float32), 0.1, 1.9)
    gate_weight = scatter_about(keys[4], (EXPERTS, D, FF), (3.0 / D ** 0.5), 0.28125, ((0, 32), (2, 32)))
    up_weight = scatter_about(keys[5], (EXPERTS, D, FF), (3.0 / D ** 0.5), 0.28125, ((0, 32), (2, 32)))
    down_weight = scatter_about(keys[6], (EXPERTS, FF, D), (0.3 / FF ** 0.5), 0.028076172, ((0, 32), (2, 32)))
    return {"tokens": tokens, "expert_ids": expert_ids, "route_weight": route_weight, "norm_gain": norm_gain, "gate_weight": gate_weight, "up_weight": up_weight, "down_weight": down_weight}


EPS = 1e-06
LIMIT = 7.0
ALPHA = 1.702

def rms_norm(tokens, norm_gain):
    values = tokens.astype(jnp.float32)
    scale = lax.rsqrt(lax.optimization_barrier(jnp.mean(values * values, axis=-1, keepdims=True)) + EPS)
    return (values * scale * norm_gain.astype(jnp.float32)).astype(jnp.bfloat16)

def clamped_unit(gate_pre, up_pre):
    gate = jnp.minimum(gate_pre, LIMIT)
    up_part = jnp.clip(up_pre, -LIMIT, LIMIT)
    return ((up_part + 1.0) * gate * jax.nn.sigmoid(ALPHA * gate)).astype(jnp.bfloat16)

def reference(tokens, expert_ids, route_weight, norm_gain, gate_weight, up_weight, down_weight):
    normed = rms_norm(tokens, norm_gain)
    copies = TOK_EP * TOPK
    ids_blocks = expert_ids.reshape(N_EP, copies).astype(jnp.int32)
    onehot = (ids_blocks[:, :, None] == jnp.arange(EXPERTS, dtype=jnp.int32)[None, None, :]).astype(jnp.int32)
    before = jnp.cumsum(onehot, axis=1) - onehot
    position = lax.optimization_barrier(jnp.sum(before * onehot, axis=2)).astype(jnp.int32)
    block_ids = jnp.broadcast_to(jnp.arange(N_EP, dtype=jnp.int32)[:, None], (N_EP, copies))
    copy_token = (block_ids * TOK_EP + jnp.arange(copies, dtype=jnp.int32)[None, :] // TOPK).astype(jnp.int32)
    table = jnp.full((EXPERTS, N_EP, CAP), TOKENS, jnp.int32)
    table = table.at[ids_blocks, block_ids, position].set(copy_token)
    weight_table = jnp.zeros((EXPERTS, N_EP, CAP), jnp.float32)
    weight_table = weight_table.at[ids_blocks, block_ids, position].set(route_weight.reshape(N_EP, copies).astype(jnp.float32))
    padded = jnp.concatenate([normed, jnp.zeros((1, D), jnp.bfloat16)], axis=0)

    def one_expert(operands):
        gate_w, up_w, down_w, row_index, weights = operands
        rows = padded[row_index.reshape(-1)]
        gate_pre = jnp.dot(rows, gate_w, preferred_element_type=jnp.float32)
        up_pre = jnp.dot(rows, up_w, preferred_element_type=jnp.float32)
        hidden = clamped_unit(gate_pre, up_pre)
        result = jnp.dot(hidden, down_w, preferred_element_type=jnp.float32).astype(jnp.bfloat16)
        result = lax.optimization_barrier(result).astype(jnp.float32)
        return result * weights.reshape(-1)[:, None]
    outputs = lax.map(one_expert, (gate_weight, up_weight, down_weight, table, weight_table))
    total = jnp.zeros((TOKENS + 1, D), jnp.float32)
    total = total.at[table.reshape(-1)].add(outputs.reshape(-1, D))
    return total[:TOKENS].astype(jnp.bfloat16)
```

```python
import jax
import jax.numpy as jnp
from jax import lax
from jax.experimental import pallas as pl
from jax.experimental.pallas import tpu as pltpu
from jax.sharding import Mesh
from jax.sharding import PartitionSpec as P

EPS = 1e-06
LIMIT = 7.0
ALPHA = 1.702
F32 = jnp.float32
BF16 = jnp.bfloat16

VMEM = pl.BlockSpec(memory_space=pltpu.VMEM)
SMEM = pl.BlockSpec(memory_space=pltpu.SMEM)
HBM = pl.BlockSpec(memory_space=pltpu.HBM)


def params(mib):
    return pltpu.CompilerParams(vmem_limit_bytes=mib << 20)


def swap(x, axes):
    return lax.all_to_all(x, axes, split_axis=0, concat_axis=0, tiled=True)


def shifted(n, by):
    return [(i, (i + by) % n) for i in range(n)]


def gate_up_quarters(x_at, gate_weight, up_weight, nx):
    width, ff = gate_weight.shape
    rows = width // nx

    def kernel(at, gate, up, *refs):
        outs, sem = refs[:nx], refs[nx]
        copies = []
        for s in range(nx):
            start = lax.rem(at[0] + s, nx) * rows
            for side, src in enumerate((gate, up)):
                copies.append(
                    pltpu.make_async_copy(
                        src.at[pl.ds(start, rows)], outs[s].at[:, pl.ds(side * ff, ff)], sem.at[2 * s + side]
                    )
                )
        for copy in copies:
            copy.start()
        for copy in copies:
            copy.wait()

    return pl.pallas_call(
        kernel,
        out_shape=[jax.ShapeDtypeStruct((rows, 2 * ff), BF16)] * nx,
        in_specs=[SMEM, HBM, HBM],
        out_specs=[VMEM] * nx,
        scratch_shapes=[pltpu.SemaphoreType.DMA((2 * nx,))],
        compiler_params=params(4),
        name="gate_up_quarters",
    )(x_at, gate_weight, up_weight)


def down_quarters(x_at, down_weight, nx):
    ny, _, ff, cols = down_weight.shape

    def kernel(at, down, *refs):
        outs, sem = refs[:nx], refs[nx]
        copies = [
            pltpu.make_async_copy(down.at[:, lax.rem(at[0] + s, nx)], outs[s], sem.at[s]) for s in range(nx)
        ]
        for copy in copies:
            copy.start()
        for copy in copies:
            copy.wait()

    return pl.pallas_call(
        kernel,
        out_shape=[jax.ShapeDtypeStruct((ny, ff, cols), BF16)] * nx,
        in_specs=[SMEM, HBM],
        out_specs=[VMEM] * nx,
        scratch_shapes=[pltpu.SemaphoreType.DMA((nx,))],
        compiler_params=params(2),
        name="down_quarters",
    )(x_at, down_weight)


def partial_products(x_at, pieces, weights):
    nx = len(weights)
    ny, rows, cols = pieces.shape
    depth, wide = weights[0].shape

    def kernel(at, x, *refs):
        w, out, joined = refs[:nx], refs[nx], refs[nx + 1]
        for j in range(ny):
            joined[:, j * cols : (j + 1) * cols] = x[j]
        for s in range(nx):
            out[lax.rem(at[0] + (nx - s), nx)] = jnp.dot(
                joined[...], w[s][...], preferred_element_type=F32
            ).astype(BF16)

    return pl.pallas_call(
        kernel,
        out_shape=jax.ShapeDtypeStruct((nx, rows, wide), BF16),
        in_specs=[SMEM, VMEM] + [VMEM] * nx,
        out_specs=VMEM,
        scratch_shapes=[pltpu.VMEM((rows, depth), BF16)],
        compiler_params=params(16),
        cost_estimate=pl.CostEstimate(flops=2 * nx * rows * depth * wide, bytes_accessed=4 << 20, transcendentals=0),
        name="partial_products",
    )(x_at, pieces, *weights)


def hidden_units(parts, copies):
    nx, rows, wide = parts.shape
    ff = wide // 2

    def kernel(p, out):
        total = p[0].astype(F32)
        for j in range(1, nx):
            total += p[j].astype(F32)
        gate = jnp.minimum(total[:, :ff], LIMIT)
        up_part = jnp.clip(total[:, ff:], -LIMIT, LIMIT)
        hidden = ((up_part + 1.0) * gate * jax.nn.sigmoid(ALPHA * gate)).astype(BF16)
        for j in range(copies):
            out[j] = hidden

    return pl.pallas_call(
        kernel,
        out_shape=jax.ShapeDtypeStruct((copies, rows, ff), BF16),
        in_specs=[VMEM],
        out_specs=VMEM,
        compiler_params=params(8),
        name="hidden_units",
    )(parts)


def from_neighbours(blocks, axis):
    n = len(blocks)
    order = [1, n - 1] + list(range(2, n - 1))
    moved = {s: lax.ppermute(blocks[s], axis, shifted(n, s)) for s in order}
    return [blocks[0]] + [moved[s] for s in range(1, n)]


def own_columns(tokens, norm_gain, cols, index):
    values = tokens.astype(F32)
    scale = lax.rsqrt(jnp.mean(values * values, axis=-1, keepdims=True) + EPS)
    own = lax.dynamic_slice_in_dim(tokens, index * cols, cols, 1).astype(F32)
    gain = lax.dynamic_slice_in_dim(norm_gain, index * cols, cols, 0)
    return (own * scale * gain).astype(BF16)


def on_device(tokens, expert_ids, route_weight, norm_gain, gate_weight, up_weight, down_weight):
    nz, nc, ny, nx = (lax.axis_size(a) for a in ("z", "c", "y", "x"))
    x_at, y_at = lax.axis_index("x"), lax.axis_index("y")
    at = x_at.reshape(1).astype(jnp.int32)
    rows, width = tokens.shape
    top = expert_ids.shape[1]
    experts = nz * nc * gate_weight.shape[0]
    cap = 5 * rows * top // (4 * experts)
    room = -(-cap // 16) * 16
    slots = experts * room
    cols = width // (nx * ny)
    ff = gate_weight.shape[2]

    pair = gate_up_quarters(at, gate_weight[0], up_weight[0], nx)
    down = down_quarters(at, down_weight.reshape(ny, nx, ff, cols), nx)

    own = own_columns(tokens, norm_gain, cols, x_at * ny + y_at)
    expert = jnp.arange(experts, dtype=jnp.int32)
    named = jnp.any(expert_ids[:, :, None] == expert, axis=1)
    earlier = jnp.arange(rows)[:, None] > jnp.arange(rows)[None, :]
    before = jnp.dot(earlier.astype(BF16), named.astype(BF16), preferred_element_type=F32)
    dest = [
        expert_ids[:, k] * room
        + jnp.sum(jnp.where(expert_ids[:, k, None] == expert, before, 0.0), axis=1).astype(jnp.int32)
        for k in range(top)
    ]
    slot = jnp.arange(slots, dtype=jnp.int32)
    pick = jnp.any(jnp.stack([slot[:, None] == d[None, :] for d in dest]), axis=0).astype(BF16)
    buffer = jnp.dot(pick, own, preferred_element_type=F32).astype(BF16)

    buffer = swap(buffer.reshape(nz, nc * room, cols), "z").reshape(nz, nc, room, cols)
    buffer = swap(jnp.swapaxes(buffer, 0, 1).reshape(nc, nz * room, cols), "c").reshape(slots, cols)

    pair, buffer = lax.optimization_barrier((pair, buffer))
    pieces = swap(jnp.broadcast_to(buffer[None], (ny, slots, cols)), "y")
    pair = from_neighbours(pair, "x")
    parts = swap(partial_products(at, pieces, pair), "x")

    hidden = hidden_units(parts, ny)
    down, hidden = lax.optimization_barrier((down, hidden))
    pieces = swap(hidden, "y")
    down = [d.reshape(ny * ff, cols) for d in from_neighbours(down, "x")]
    parts = swap(partial_products(at, pieces, down), "x")
    result = jnp.sum(parts.astype(F32), axis=0).astype(BF16)

    result = swap(result.reshape(nc, nz * room, cols), "c").reshape(nc, nz, room, cols)
    back = swap(jnp.swapaxes(result, 0, 1).reshape(nz, nc * room, cols), "z").reshape(slots, cols)
    mixed = 0.0
    for k in range(top):
        chosen = (dest[k][:, None] == slot[None, :]).astype(BF16)
        mixed += jnp.dot(chosen, back, preferred_element_type=F32) * route_weight[:, k, None]
    return mixed.astype(BF16)


def solution(mesh):
    torus = Mesh(mesh.devices.reshape(mesh.shape["ep"] // 2, 2, 8, 4), ("z", "c", "y", "x"))
    ep, tp = ("z", "c"), ("y", "x")
    in_specs = (
        P(ep, None),
        P(ep, None),
        P(ep, None),
        P(),
        P(ep, None, tp),
        P(ep, None, tp),
        P(ep, None, tp),
    )
    return jax.shard_map(
        on_device, mesh=torus, in_specs=in_specs, out_specs=P(ep, tp), check_vma=False
    )
```

```python
import jax
import jax.numpy as jnp
from jax import lax
from jax.experimental import pallas as pl
from jax.experimental.pallas import tpu as pltpu
from jax.sharding import Mesh
from jax.sharding import PartitionSpec as P


EPS = 1e-06
LIMIT = 7.0
ALPHA = 1.702
F32 = jnp.float32
BF16 = jnp.bfloat16

VMEM = pl.BlockSpec(memory_space=pltpu.VMEM)
SMEM = pl.BlockSpec(memory_space=pltpu.SMEM)
HBM = pl.BlockSpec(memory_space=pltpu.HBM)


def params(mib):
    return pltpu.CompilerParams(vmem_limit_bytes=mib << 20)


def swap(x, axes):
    return lax.all_to_all(x, axes, split_axis=0, concat_axis=0, tiled=True)


def shifted(n, by):
    return [(i, (i + by) % n) for i in range(n)]


def weight_quarters(x_at, gate_weight, up_weight, down_weight, nx):
    width, ff = gate_weight.shape
    ny, _, _, cols = down_weight.shape
    rows = width // nx

    def kernel(at, gate, up, down, *refs):
        outs, sem = refs[: 2 * nx], refs[2 * nx]
        copies = []
        for s in range(nx):
            quarter = lax.rem(at[0] + s, nx)
            for side, src in enumerate((gate, up)):
                copies.append(
                    pltpu.make_async_copy(
                        src.at[pl.ds(quarter * rows, rows)],
                        outs[s].at[:, pl.ds(side * ff, ff)],
                        sem.at[3 * s + side],
                    )
                )
            copies.append(pltpu.make_async_copy(down.at[:, quarter], outs[nx + s], sem.at[3 * s + 2]))
        for copy in copies:
            copy.start()
        for copy in copies:
            copy.wait()

    return pl.pallas_call(
        kernel,
        out_shape=[jax.ShapeDtypeStruct((rows, 2 * ff), BF16)] * nx
        + [jax.ShapeDtypeStruct((ny, ff, cols), BF16)] * nx,
        in_specs=[SMEM, HBM, HBM, HBM],
        out_specs=[VMEM] * (2 * nx),
        scratch_shapes=[pltpu.SemaphoreType.DMA((3 * nx,))],
        compiler_params=params(4),
        name="weight_quarters",
    )(x_at, gate_weight, up_weight, down_weight)


def dispatch(tp_at, tokens, ids, gain, experts, room, cols):
    rows, width = tokens.shape
    top = ids.shape[0]
    slots = experts * room

    def kernel(at, tok, ids_ref, gain_ref, out, dest_ref):
        values = tok[...].astype(F32)
        scale = lax.rsqrt(jnp.sum(values * values, axis=-1, keepdims=True) * (1.0 / width) + EPS)
        start = pl.multiple_of(at[0] * cols, cols)
        own = (tok[:, pl.ds(start, cols)].astype(F32) * scale * gain_ref[:, pl.ds(start, cols)]).astype(BF16)
        expert = lax.broadcasted_iota(jnp.int32, (experts, rows), 0)
        here = [ids_ref[k : k + 1, :] == expert for k in range(top)]
        named = sum(h.astype(F32) for h in here).astype(BF16)
        earlier = lax.broadcasted_iota(jnp.int32, (rows, rows), 0) < lax.broadcasted_iota(
            jnp.int32, (rows, rows), 1
        )
        before = jnp.dot(named, earlier.astype(F32).astype(BF16), preferred_element_type=F32)
        slot = lax.broadcasted_iota(jnp.int32, (slots, rows), 0)
        pick = None
        for k in range(top):
            place = jnp.sum(jnp.where(here[k], before, 0.0), axis=0, keepdims=True).astype(jnp.int32)
            dest = ids_ref[k : k + 1, :] * room + place
            dest_ref[k : k + 1, :] = dest
            hit = (slot == dest).astype(F32)
            pick = hit if pick is None else pick + hit
        out[...] = jnp.dot(pick.astype(BF16), own, preferred_element_type=F32).astype(BF16)

    return pl.pallas_call(
        kernel,
        out_shape=[jax.ShapeDtypeStruct((slots, cols), BF16), jax.ShapeDtypeStruct((top, rows), jnp.int32)],
        in_specs=[SMEM, VMEM, VMEM, VMEM],
        out_specs=[VMEM, VMEM],
        compiler_params=params(12),
        name="dispatch",
    )(tp_at, tokens, ids, gain)


def fan_out(arrived, copies):
    nz, nc, room, cols = arrived.shape

    def kernel(x, out):
        for c in range(nc):
            block = x[:, c].reshape(nz * room, cols)
            for j in range(copies):
                out[c * copies + j] = block

    return pl.pallas_call(
        kernel,
        out_shape=jax.ShapeDtypeStruct((nc * copies, nz * room, cols), BF16),
        in_specs=[VMEM],
        out_specs=VMEM,
        compiler_params=params(4),
        name="fan_out",
    )(arrived)


def partial_products(x_at, pieces, weights, groups_in, groups_out):
    nx = len(weights)
    blocks, some, cols = pieces.shape
    depth, wide = weights[0].shape
    rows, ny = some * groups_in, blocks // groups_in
    share = rows // groups_out

    def kernel(at, x, *refs):
        w, out, joined = refs[:nx], refs[nx], refs[nx + 1]
        for g in range(groups_in):
            for j in range(ny):
                joined[g * some : (g + 1) * some, j * cols : (j + 1) * cols] = x[g * ny + j]
        for s in range(nx):
            place = lax.rem(at[0] + (nx - s), nx)
            product = jnp.dot(joined[...], w[s][...], preferred_element_type=F32).astype(BF16)
            for g in range(groups_out):
                out[g * nx + place] = product[g * share : (g + 1) * share]

    return pl.pallas_call(
        kernel,
        out_shape=jax.ShapeDtypeStruct((groups_out * nx, share, wide), BF16),
        in_specs=[SMEM, VMEM] + [VMEM] * nx,
        out_specs=VMEM,
        scratch_shapes=[pltpu.VMEM((rows, depth), BF16)],
        compiler_params=params(16),
        cost_estimate=pl.CostEstimate(flops=2 * nx * rows * depth * wide, bytes_accessed=4 << 20, transcendentals=0),
        name="partial_products",
    )(x_at, pieces, *weights)


def hidden_units(parts, copies):
    nx, rows, wide = parts.shape
    ff = wide // 2

    def kernel(p, out):
        total = p[0].astype(F32)
        for j in range(1, nx):
            total += p[j].astype(F32)
        gate = jnp.minimum(total[:, :ff], LIMIT)
        up_part = jnp.clip(total[:, ff:], -LIMIT, LIMIT)
        hidden = ((up_part + 1.0) * gate * jax.nn.sigmoid(ALPHA * gate)).astype(BF16)
        for j in range(copies):
            out[j] = hidden

    return pl.pallas_call(
        kernel,
        out_shape=jax.ShapeDtypeStruct((copies, rows, ff), BF16),
        in_specs=[VMEM],
        out_specs=VMEM,
        compiler_params=params(8),
        name="hidden_units",
    )(parts)


def from_neighbours(blocks, axis):
    n = len(blocks)
    order = dict.fromkeys([1, n - 1] + list(range(2, n - 1)))
    moved = {s: lax.ppermute(blocks[s], axis, shifted(n, s)) for s in order}
    return [blocks[0]] + [moved[s] for s in range(1, n)]


def add_up(parts, groups, blocks):
    total, rows, cols = parts.shape
    terms = total // groups

    def kernel(p, out):
        for g in range(groups):
            value = p[g * terms].astype(F32)
            for j in range(1, terms):
                value += p[g * terms + j].astype(F32)
            out[:, g] = value.astype(BF16).reshape(blocks, rows // blocks, cols)

    return pl.pallas_call(
        kernel,
        out_shape=jax.ShapeDtypeStruct((blocks, groups, rows // blocks, cols), BF16),
        in_specs=[VMEM],
        out_specs=VMEM,
        compiler_params=params(4),
        name="add_up",
    )(parts)


def on_device(tokens, expert_ids, route_weight, norm_gain, gate_weight, up_weight, down_weight):
    nz, nc, ny, nx = (lax.axis_size(a) for a in ("z", "c", "y", "x"))
    x_at, y_at = lax.axis_index("x"), lax.axis_index("y")
    at = x_at.reshape(1).astype(jnp.int32)
    tp_at = (x_at * ny + y_at).reshape(1).astype(jnp.int32)
    rows, width = tokens.shape
    top = expert_ids.shape[1]
    experts = nz * nc * gate_weight.shape[0]
    cap = 5 * rows * top // (4 * experts)
    room = -(-cap // 16) * 16
    slots = experts * room
    cols = width // (nx * ny)
    ff = gate_weight.shape[2]

    buffer, dest = dispatch(tp_at, tokens, expert_ids.T, norm_gain.reshape(1, width), experts, room, cols)
    gate_weight, buffer = lax.optimization_barrier((gate_weight, buffer))
    quarters = weight_quarters(
        at, gate_weight[0], up_weight[0], down_weight.reshape(ny, nx, ff, cols), nx
    )
    pair, down = quarters[:nx], quarters[nx:]

    arrived = swap(buffer.reshape(nz, nc * room, cols), "z").reshape(nz, nc, room, cols)
    pair = from_neighbours(pair, "x")
    blocks = fan_out(arrived, ny)
    pieces = swap(blocks, ("c", "y"))
    down = [d.reshape(ny * ff, cols) for d in from_neighbours(down, "x")]
    parts = partial_products(at, pieces, pair, nc, 1)
    parts = swap(parts, "x")

    hidden = hidden_units(parts, ny)
    pieces = swap(hidden, "y")
    parts = swap(partial_products(at, pieces, down, 1, nc), ("c", "x"))

    back = swap(add_up(parts, nc, nz).reshape(nz, nc * room, cols), "z").reshape(slots, cols)
    slot = jnp.arange(slots, dtype=jnp.int32)
    mixed = 0.0
    for k in range(top):
        chosen = (dest[k][:, None] == slot[None, :]).astype(BF16)
        mixed += jnp.dot(chosen, back, preferred_element_type=F32) * route_weight[:, k, None]
    return mixed.astype(BF16)


def solution(mesh):
    torus = Mesh(mesh.devices.reshape(mesh.shape["ep"] // 2, 2, 8, 4), ("z", "c", "y", "x"))
    ep, tp = ("z", "c"), ("y", "x")
    in_specs = (
        P(ep, None),
        P(ep, None),
        P(ep, None),
        P(),
        P(ep, None, tp),
        P(ep, None, tp),
        P(ep, None, tp),
    )

    return jax.shard_map(on_device, mesh=torus, in_specs=in_specs, out_specs=P(ep, tp), check_vma=False)
```

```python
import jax
import jax.numpy as jnp
from jax import lax
from jax.experimental import pallas as pl
from jax.experimental.pallas import tpu as pltpu
from jax.sharding import Mesh
from jax.sharding import PartitionSpec as P


EPS = 1e-06
LIMIT = 7.0
ALPHA = 1.702
F32 = jnp.float32
BF16 = jnp.bfloat16

VMEM = pl.BlockSpec(memory_space=pltpu.VMEM)
SMEM = pl.BlockSpec(memory_space=pltpu.SMEM)
HBM = pl.BlockSpec(memory_space=pltpu.HBM)


def params(mib):
    return pltpu.CompilerParams(vmem_limit_bytes=mib << 20)


def swap(x, axes):
    return lax.all_to_all(x, axes, split_axis=0, concat_axis=0, tiled=True)


def shifted(n, by):
    return [(i, (i + by) % n) for i in range(n)]


def weight_quarters(x_at, gate_weight, up_weight, down_weight, nx):
    width, ff = gate_weight.shape
    ny, _, _, cols = down_weight.shape
    rows = width // nx
    each = 2 + ny

    def kernel(at, gate, up, down, *refs):
        outs, sem = refs[:nx], refs[nx]
        copies = []
        for s in range(nx):
            quarter = lax.rem(at[0] + s, nx)
            for side, src in enumerate((gate, up)):
                copies.append(
                    pltpu.make_async_copy(
                        src.at[pl.ds(quarter * rows, rows)],
                        outs[s].at[:, pl.ds(side * ff, ff)],
                        sem.at[each * s + side],
                    )
                )
            for j in range(ny):
                copies.append(
                    pltpu.make_async_copy(
                        down.at[j, quarter],
                        outs[s].at[pl.ds(j * ff, ff), pl.ds(2 * ff, cols)],
                        sem.at[each * s + 2 + j],
                    )
                )
        for copy in copies:
            copy.start()
        for copy in copies:
            copy.wait()

    return pl.pallas_call(
        kernel,
        out_shape=[jax.ShapeDtypeStruct((rows, 2 * ff + cols), BF16)] * nx,
        in_specs=[SMEM, HBM, HBM, HBM],
        out_specs=[HBM] * nx,
        scratch_shapes=[pltpu.SemaphoreType.DMA((each * nx,))],
        compiler_params=params(2),
        name="weight_quarters",
    )(x_at, gate_weight, up_weight, down_weight)


def dispatch(tp_at, tokens, ids, gain, experts, room, cols):
    rows, width = tokens.shape
    top = ids.shape[0]
    slots = experts * room
    chunks = 4 if rows % 64 == 0 else 1
    step = rows // chunks

    def kernel(at, tok_hbm, ids_hbm, gain_hbm, out, dest_ref, tok, ids_ref, gain_ref, own_ref, sem):
        start = pl.multiple_of(at[0] * cols, cols)
        small = [
            pltpu.make_async_copy(ids_hbm, ids_ref, sem.at[chunks]),
            pltpu.make_async_copy(gain_hbm.at[:, pl.ds(start, cols)], gain_ref, sem.at[chunks + 1]),
        ]
        large = [
            pltpu.make_async_copy(tok_hbm.at[pl.ds(i * step, step)], tok.at[pl.ds(i * step, step)], sem.at[i])
            for i in range(chunks)
        ]
        for copy in small + large:
            copy.start()
        for copy in small:
            copy.wait()
        expert = lax.broadcasted_iota(jnp.int32, (experts, rows), 0)
        here = [ids_ref[k : k + 1, :] == expert for k in range(top)]
        named = sum(h.astype(F32) for h in here).astype(BF16)
        earlier = lax.broadcasted_iota(jnp.int32, (rows, rows), 0) < lax.broadcasted_iota(
            jnp.int32, (rows, rows), 1
        )
        before = jnp.dot(named, earlier.astype(F32).astype(BF16), preferred_element_type=F32)
        slot = lax.broadcasted_iota(jnp.int32, (slots, rows), 0)
        pick = None
        for k in range(top):
            place = jnp.sum(jnp.where(here[k], before, 0.0), axis=0, keepdims=True).astype(jnp.int32)
            dest = ids_ref[k : k + 1, :] * room + place
            dest_ref[k : k + 1, :] = dest
            hit = (slot == dest).astype(F32)
            pick = hit if pick is None else pick + hit
        pick = pick.astype(BF16)
        for i in range(chunks):
            large[i].wait()
            at_rows = slice(i * step, (i + 1) * step)
            values = tok[at_rows, :].astype(F32)
            scale = lax.rsqrt(jnp.sum(values * values, axis=-1, keepdims=True) * (1.0 / width) + EPS)
            own = tok[at_rows, pl.ds(start, cols)].astype(F32)
            own_ref[at_rows, :] = (own * scale * gain_ref[...]).astype(BF16)
        out[...] = jnp.dot(pick, own_ref[...], preferred_element_type=F32).astype(BF16)

    return pl.pallas_call(
        kernel,
        out_shape=[jax.ShapeDtypeStruct((slots, cols), BF16), jax.ShapeDtypeStruct((top, rows), jnp.int32)],
        in_specs=[SMEM, HBM, HBM, HBM],
        out_specs=[VMEM, VMEM],
        scratch_shapes=[
            pltpu.VMEM((rows, width), BF16),
            pltpu.VMEM((top, rows), jnp.int32),
            pltpu.VMEM((1, cols), F32),
            pltpu.VMEM((rows, cols), BF16),
            pltpu.SemaphoreType.DMA((chunks + 2,)),
        ],
        compiler_params=params(12),
        name="dispatch",
    )(tp_at, tokens, ids, gain)


def fan_out(arrived, copies):
    nz, nc, room, cols = arrived.shape

    def kernel(x, out):
        for c in range(nc):
            block = x[:, c].reshape(nz * room, cols)
            for j in range(copies):
                out[c * copies + j] = block

    return pl.pallas_call(
        kernel,
        out_shape=jax.ShapeDtypeStruct((nc * copies, nz * room, cols), BF16),
        in_specs=[VMEM],
        out_specs=VMEM,
        compiler_params=params(4),
        name="fan_out",
    )(arrived)


def join(pieces, groups):
    blocks, some, cols = pieces.shape
    rows, ny = some * groups, blocks // groups

    def kernel(x, out):
        for g in range(groups):
            for j in range(ny):
                out[g * some : (g + 1) * some, j * cols : (j + 1) * cols] = x[g * ny + j]

    return pl.pallas_call(
        kernel,
        out_shape=jax.ShapeDtypeStruct((rows, ny * cols), BF16),
        in_specs=[VMEM],
        out_specs=VMEM,
        compiler_params=params(4),
        name="join",
    )(pieces)


def partial_products(x_at, left, weights, first, wide, groups):
    nx = len(weights)
    rows, depth = left.shape
    share = rows // groups
    pairs = 256 // wide

    def kernel(at, x, *refs):
        w, out = refs[:nx], refs[nx]
        for s in range(0, nx, pairs):
            right = [w[s + i][:, first : first + wide] for i in range(pairs)]
            right = right[0] if pairs == 1 else jnp.concatenate(right, axis=1)
            product = jnp.dot(x[...], right, preferred_element_type=F32).astype(BF16)
            for i in range(pairs):
                place = lax.rem(at[0] + (nx - s - i), nx)
                for g in range(groups):
                    out[g * nx + place] = product[g * share : (g + 1) * share, i * wide : (i + 1) * wide]

    return pl.pallas_call(
        kernel,
        out_shape=jax.ShapeDtypeStruct((groups * nx, share, wide), BF16),
        in_specs=[SMEM, VMEM] + [VMEM] * nx,
        out_specs=VMEM,
        compiler_params=params(16),
        cost_estimate=pl.CostEstimate(flops=2 * nx * rows * depth * wide, bytes_accessed=4 << 20, transcendentals=0),
        name="partial_products",
    )(x_at, left, *weights)


def hidden_units(parts, copies):
    nx, rows, wide = parts.shape
    ff = wide // 2

    def kernel(p, out):
        total = p[0].astype(F32)
        for j in range(1, nx):
            total += p[j].astype(F32)
        gate = jnp.minimum(total[:, :ff], LIMIT)
        up_part = jnp.clip(total[:, ff:], -LIMIT, LIMIT)
        hidden = ((up_part + 1.0) * gate * jax.nn.sigmoid(ALPHA * gate)).astype(BF16)
        for j in range(copies):
            out[j] = hidden

    return pl.pallas_call(
        kernel,
        out_shape=jax.ShapeDtypeStruct((copies, rows, ff), BF16),
        in_specs=[VMEM],
        out_specs=VMEM,
        compiler_params=params(8),
        name="hidden_units",
    )(parts)


def from_neighbours(blocks, axis):
    n = len(blocks)
    order = dict.fromkeys([1, n - 1] + list(range(2, n - 1)))
    moved = {s: lax.ppermute(blocks[s], axis, shifted(n, s)) for s in order}
    return [blocks[0]] + [moved[s] for s in range(1, n)]


def add_up(parts, groups, blocks):
    total, rows, cols = parts.shape
    terms = total // groups

    def kernel(p, out):
        for g in range(groups):
            value = p[g * terms].astype(F32)
            for j in range(1, terms):
                value += p[g * terms + j].astype(F32)
            out[:, g] = value.astype(BF16).reshape(blocks, rows // blocks, cols)

    return pl.pallas_call(
        kernel,
        out_shape=jax.ShapeDtypeStruct((blocks, groups, rows // blocks, cols), BF16),
        in_specs=[VMEM],
        out_specs=VMEM,
        compiler_params=params(4),
        name="add_up",
    )(parts)


def combine(back, dest, route):
    slots, cols = back.shape
    top, rows = dest.shape

    def kernel(x, dest_ref, route_ref, out):
        slot = lax.broadcasted_iota(jnp.int32, (slots, rows), 0)
        total = None
        for k in range(top):
            chosen = (slot == dest_ref[k : k + 1, :]).astype(F32).astype(BF16)
            copy = lax.dot_general(chosen, x[...], (((0,), (0,)), ((), ())), preferred_element_type=F32)
            copy = copy * route_ref[k]
            total = copy if total is None else total + copy
        out[...] = total.astype(BF16)

    return pl.pallas_call(
        kernel,
        out_shape=jax.ShapeDtypeStruct((rows, cols), BF16),
        in_specs=[VMEM, VMEM, VMEM],
        out_specs=VMEM,
        compiler_params=params(8),
        name="combine",
    )(back, dest, route)


def on_device(tokens, expert_ids, route_weight, norm_gain, gate_weight, up_weight, down_weight):
    nz, nc, ny, nx = (lax.axis_size(a) for a in ("z", "c", "y", "x"))
    x_at, y_at = lax.axis_index("x"), lax.axis_index("y")
    at = x_at.reshape(1).astype(jnp.int32)
    tp_at = (x_at * ny + y_at).reshape(1).astype(jnp.int32)
    rows, width = tokens.shape
    top = expert_ids.shape[1]
    experts = nz * nc * gate_weight.shape[0]
    cap = 5 * rows * top // (4 * experts)
    room = -(-cap // 16) * 16
    slots = experts * room
    cols = width // (nx * ny)
    ff = gate_weight.shape[2]

    buffer, dest = dispatch(tp_at, tokens, expert_ids.T, norm_gain.reshape(1, width), experts, room, cols)
    gate_weight, buffer = lax.optimization_barrier((gate_weight, buffer))
    weights = weight_quarters(
        at, gate_weight[0], up_weight[0], down_weight.reshape(ny, nx, ff, cols), nx
    )

    arrived = swap(buffer.reshape(nz, nc * room, cols), "z").reshape(nz, nc, room, cols)
    weights = from_neighbours(weights, "x")
    blocks = fan_out(arrived, ny)
    pieces = swap(blocks, ("c", "y"))
    left = join(pieces, nc)
    parts = partial_products(at, left, weights, 0, 2 * ff, 1)
    parts = swap(parts, "x")

    hidden = hidden_units(parts, ny)
    pieces = swap(hidden, "y")
    parts = partial_products(at, join(pieces, 1), weights, 2 * ff, cols, nc)
    parts = swap(parts, ("c", "x"))

    result = add_up(parts, nc, nz).reshape(nz, nc * room, cols)
    back = swap(result, "z").reshape(slots, cols)
    return combine(back, dest, jnp.broadcast_to(route_weight.T[:, :, None], (top, rows, cols)))


def solution(mesh):
    torus = Mesh(mesh.devices.reshape(mesh.shape["ep"] // 2, 2, 8, 4), ("z", "c", "y", "x"))
    ep, tp = ("z", "c"), ("y", "x")
    in_specs = (
        P(ep, None),
        P(ep, None),
        P(ep, None),
        P(),
        P(ep, None, tp),
        P(ep, None, tp),
        P(ep, None, tp),
    )

    return jax.shard_map(on_device, mesh=torus, in_specs=in_specs, out_specs=P(ep, tp), check_vma=False)
```

```python
import jax
import jax.numpy as jnp
from jax import lax
from jax.experimental import pallas as pl
from jax.experimental.pallas import tpu as pltpu
from jax.sharding import Mesh
from jax.sharding import PartitionSpec as P


EPS = 1e-06
LIMIT = 7.0
ALPHA = 1.702
F32 = jnp.float32
BF16 = jnp.bfloat16

VMEM = pl.BlockSpec(memory_space=pltpu.VMEM)
SMEM = pl.BlockSpec(memory_space=pltpu.SMEM)
HBM = pl.BlockSpec(memory_space=pltpu.HBM)


def params(mib):
    return pltpu.CompilerParams(vmem_limit_bytes=mib << 20)


def swap(x, axes):
    return lax.all_to_all(x, axes, split_axis=0, concat_axis=0, tiled=True)


def shifted(n, by):
    return [(i, (i + by) % n) for i in range(n)]


def weight_quarters(x_at, gate_weight, up_weight, down_weight, nx):
    width, ff = gate_weight.shape
    ny, _, _, cols = down_weight.shape
    rows = width // nx
    each = 2 + ny

    def kernel(at, gate, up, down, *refs):
        outs, sem = refs[:nx], refs[nx]
        copies = []
        for s in range(nx):
            quarter = lax.rem(at[0] + s, nx)
            for side, src in enumerate((gate, up)):
                copies.append(
                    pltpu.make_async_copy(
                        src.at[pl.ds(quarter * rows, rows)],
                        outs[s].at[:, pl.ds(side * ff, ff)],
                        sem.at[each * s + side],
                    )
                )
            for j in range(ny):
                copies.append(
                    pltpu.make_async_copy(
                        down.at[j, quarter],
                        outs[s].at[pl.ds(j * ff, ff), pl.ds(2 * ff, cols)],
                        sem.at[each * s + 2 + j],
                    )
                )
        for copy in copies:
            copy.start()
        for copy in copies:
            copy.wait()

    return pl.pallas_call(
        kernel,
        out_shape=[jax.ShapeDtypeStruct((rows, 2 * ff + cols), BF16)] * nx,
        in_specs=[SMEM, HBM, HBM, HBM],
        out_specs=[HBM] * nx,
        scratch_shapes=[pltpu.SemaphoreType.DMA((each * nx,))],
        compiler_params=params(2),
        name="weight_quarters",
    )(x_at, gate_weight, up_weight, down_weight)


def dispatch(tp_at, tokens, ids, gain, experts, room, cols):
    rows, width = tokens.shape
    top = ids.shape[0]
    slots = experts * room

    def kernel(at, tok, ids_ref, gain_ref, out, dest_ref):
        values = tok[...].astype(F32)
        scale = lax.rsqrt(jnp.sum(values * values, axis=-1, keepdims=True) * (1.0 / width) + EPS)
        start = pl.multiple_of(at[0] * cols, cols)
        own = (tok[:, pl.ds(start, cols)].astype(F32) * scale * gain_ref[:, pl.ds(start, cols)]).astype(BF16)
        expert = lax.broadcasted_iota(jnp.int32, (experts, rows), 0)
        here = [ids_ref[k : k + 1, :] == expert for k in range(top)]
        named = sum(h.astype(F32) for h in here).astype(BF16)
        earlier = lax.broadcasted_iota(jnp.int32, (rows, rows), 0) < lax.broadcasted_iota(
            jnp.int32, (rows, rows), 1
        )
        before = jnp.dot(named, earlier.astype(F32).astype(BF16), preferred_element_type=F32)
        slot = lax.broadcasted_iota(jnp.int32, (slots, rows), 0)
        pick = None
        for k in range(top):
            place = jnp.sum(jnp.where(here[k], before, 0.0), axis=0, keepdims=True).astype(jnp.int32)
            dest = ids_ref[k : k + 1, :] * room + place
            dest_ref[k : k + 1, :] = dest
            hit = (slot == dest).astype(F32)
            pick = hit if pick is None else pick + hit
        out[...] = jnp.dot(pick.astype(BF16), own, preferred_element_type=F32).astype(BF16)

    return pl.pallas_call(
        kernel,
        out_shape=[jax.ShapeDtypeStruct((slots, cols), BF16), jax.ShapeDtypeStruct((top, rows), jnp.int32)],
        in_specs=[SMEM, VMEM, VMEM, VMEM],
        out_specs=[VMEM, VMEM],
        compiler_params=params(12),
        name="dispatch",
    )(tp_at, tokens, ids, gain)


def by_core(arrived):
    nz, nc, room, cols = arrived.shape

    def kernel(x, out):
        for c in range(nc):
            out[c] = x[:, c].reshape(nz * room, cols)

    return pl.pallas_call(
        kernel,
        out_shape=jax.ShapeDtypeStruct((nc, nz * room, cols), BF16),
        in_specs=[VMEM],
        out_specs=VMEM,
        compiler_params=params(4),
        name="by_core",
    )(arrived)


def used_slots(slots, rows, cap, room, slots_first):
    shape, at = ((slots, rows), 0) if slots_first else ((rows, slots), 1)
    slot = lax.broadcasted_iota(jnp.int32, shape, at)
    place = slot & (room - 1)
    row = lax.shift_right_logical(slot, room.bit_length() - 1) * cap + place
    hit = (row == lax.broadcasted_iota(jnp.int32, shape, 1 - at)) & (place < cap)
    return hit.astype(F32).astype(BF16)


def close_up(arrived, cap, room):
    slots, cols = arrived.shape
    rows = slots // room * cap

    def kernel(x, out):
        pick = used_slots(slots, rows, cap, room, False)
        out[...] = jnp.dot(pick, x[...], preferred_element_type=F32).astype(BF16)

    return pl.pallas_call(
        kernel,
        out_shape=jax.ShapeDtypeStruct((rows, cols), BF16),
        in_specs=[VMEM],
        out_specs=VMEM,
        compiler_params=params(4),
        name="close_up",
    )(arrived)


def join(pieces):
    ny, rows, cols = pieces.shape

    def kernel(x, out):
        for j in range(ny):
            out[:, j * cols : (j + 1) * cols] = x[j]

    return pl.pallas_call(
        kernel,
        out_shape=jax.ShapeDtypeStruct((rows, ny * cols), BF16),
        in_specs=[VMEM],
        out_specs=VMEM,
        compiler_params=params(4),
        name="join",
    )(pieces)


def partial_products(x_at, left, weights, first, wide, groups):
    nx = len(weights)
    rows, depth = left.shape
    share = rows // groups
    pairs = 256 // wide

    def kernel(at, x, *refs):
        w, out = refs[:nx], refs[nx]
        for s in range(0, nx, pairs):
            right = [w[s + i][:, first : first + wide] for i in range(pairs)]
            right = right[0] if pairs == 1 else jnp.concatenate(right, axis=1)
            product = jnp.dot(x[...], right, preferred_element_type=F32).astype(BF16)
            for i in range(pairs):
                place = lax.rem(at[0] + (nx - s - i), nx)
                for g in range(groups):
                    out[g * nx + place] = product[g * share : (g + 1) * share, i * wide : (i + 1) * wide]

    return pl.pallas_call(
        kernel,
        out_shape=jax.ShapeDtypeStruct((groups * nx, share, wide), BF16),
        in_specs=[SMEM, VMEM] + [VMEM] * nx,
        out_specs=VMEM,
        compiler_params=params(16),
        cost_estimate=pl.CostEstimate(flops=2 * nx * rows * depth * wide, bytes_accessed=4 << 20, transcendentals=0),
        name="partial_products",
    )(x_at, left, *weights)


def hidden_units(parts):
    nx, rows, wide = parts.shape
    ff = wide // 2

    def kernel(p, out):
        total = p[0].astype(F32)
        for j in range(1, nx):
            total += p[j].astype(F32)
        gate = jnp.minimum(total[:, :ff], LIMIT)
        up_part = jnp.clip(total[:, ff:], -LIMIT, LIMIT)
        out[...] = ((up_part + 1.0) * gate * jax.nn.sigmoid(ALPHA * gate)).astype(BF16)

    return pl.pallas_call(
        kernel,
        out_shape=jax.ShapeDtypeStruct((rows, ff), BF16),
        in_specs=[VMEM],
        out_specs=VMEM,
        compiler_params=params(8),
        name="hidden_units",
    )(parts)


def from_neighbours(blocks, axis):
    n = len(blocks)
    order = dict.fromkeys([1, n - 1] + list(range(2, n - 1)))
    moved = {s: lax.ppermute(blocks[s], axis, shifted(n, s)) for s in order}
    return [blocks[0]] + [moved[s] for s in range(1, n)]


def add_up(parts, groups, blocks, cap, room):
    total, rows, cols = parts.shape
    terms = total // groups

    def kernel(p, out):
        spread = used_slots(blocks * room, rows, cap, room, True)
        for g in range(groups):
            value = p[g * terms].astype(F32)
            for j in range(1, terms):
                value += p[g * terms + j].astype(F32)
            value = jnp.dot(spread, value.astype(BF16), preferred_element_type=F32).astype(BF16)
            out[:, g] = value.reshape(blocks, room, cols)

    return pl.pallas_call(
        kernel,
        out_shape=jax.ShapeDtypeStruct((blocks, groups, room, cols), BF16),
        in_specs=[VMEM],
        out_specs=VMEM,
        compiler_params=params(4),
        name="add_up",
    )(parts)


def combine(back, dest, route):
    slots, cols = back.shape
    top, rows = dest.shape

    def kernel(x, dest_ref, route_ref, out):
        slot = lax.broadcasted_iota(jnp.int32, (slots, rows), 0)
        total = None
        for k in range(top):
            chosen = (slot == dest_ref[k : k + 1, :]).astype(F32).astype(BF16)
            copy = lax.dot_general(chosen, x[...], (((0,), (0,)), ((), ())), preferred_element_type=F32)
            copy = copy * route_ref[k]
            total = copy if total is None else total + copy
        out[...] = total.astype(BF16)

    return pl.pallas_call(
        kernel,
        out_shape=jax.ShapeDtypeStruct((rows, cols), BF16),
        in_specs=[VMEM, VMEM, VMEM],
        out_specs=VMEM,
        compiler_params=params(8),
        name="combine",
    )(back, dest, route)


def on_device(tokens, expert_ids, route_weight, norm_gain, gate_weight, up_weight, down_weight):
    nz, nc, ny, nx = (lax.axis_size(a) for a in ("z", "c", "y", "x"))
    x_at, y_at = lax.axis_index("x"), lax.axis_index("y")
    at = x_at.reshape(1).astype(jnp.int32)
    tp_at = (x_at * ny + y_at).reshape(1).astype(jnp.int32)
    rows, width = tokens.shape
    top = expert_ids.shape[1]
    experts = nz * nc * gate_weight.shape[0]
    cap = 5 * rows * top // (4 * experts)
    room = max(16, pl.next_power_of_2(cap))
    slots = experts * room
    cols = width // (nx * ny)
    ff = gate_weight.shape[2]

    buffer, dest = dispatch(tp_at, tokens, expert_ids.T, norm_gain.reshape(1, width), experts, room, cols)
    gate_weight, buffer = lax.optimization_barrier((gate_weight, buffer))
    weights = weight_quarters(
        at, gate_weight[0], up_weight[0], down_weight.reshape(ny, nx, ff, cols), nx
    )

    arrived = swap(buffer.reshape(nz, nc * room, cols), "z").reshape(nz, nc, room, cols)
    weights = from_neighbours(weights, "x")
    arrived = by_core(arrived)
    arrived = swap(arrived, "c").reshape(slots, cols)
    pieces = lax.all_gather(close_up(arrived, cap, room), "y")
    left = join(pieces)
    parts = partial_products(at, left, weights, 0, 2 * ff, 1)
    parts = swap(parts, "x")

    pieces = lax.all_gather(hidden_units(parts), "y")
    parts = partial_products(at, join(pieces), weights, 2 * ff, cols, nc)
    parts = swap(parts, ("c", "x"))

    result = add_up(parts, nc, nz, cap, room).reshape(nz, nc * room, cols)
    back = swap(result, "z").reshape(slots, cols)
    return combine(back, dest, jnp.broadcast_to(route_weight.T[:, :, None], (top, rows, cols)))


def solution(mesh):
    torus = Mesh(mesh.devices.reshape(mesh.shape["ep"] // 2, 2, 8, 4), ("z", "c", "y", "x"))
    ep, tp = ("z", "c"), ("y", "x")
    in_specs = (
        P(ep, None),
        P(ep, None),
        P(ep, None),
        P(),
        P(ep, None, tp),
        P(ep, None, tp),
        P(ep, None, tp),
    )

    return jax.shard_map(on_device, mesh=torus, in_specs=in_specs, out_specs=P(ep, tp), check_vma=False)
```

```python
import jax
import jax.numpy as jnp
from jax import lax
from jax.experimental import pallas as pl
from jax.experimental.pallas import tpu as pltpu
from jax.sharding import Mesh
from jax.sharding import PartitionSpec as P


EPS = 1e-06
LIMIT = 7.0
ALPHA = 1.702
F32 = jnp.float32
BF16 = jnp.bfloat16

VMEM = pl.BlockSpec(memory_space=pltpu.VMEM)
SMEM = pl.BlockSpec(memory_space=pltpu.SMEM)
HBM = pl.BlockSpec(memory_space=pltpu.HBM)


WHOLE = pltpu.CompilerParams(vmem_limit_bytes=67_043_328)


def params(mib):
    return pltpu.CompilerParams(vmem_limit_bytes=mib << 20)


def swap(x, axes):
    return lax.all_to_all(x, axes, split_axis=0, concat_axis=0, tiled=True)


def shifted(n, by):
    return [(i, (i + by) % n) for i in range(n)]


def weight_quarters(x_at, gate_weight, up_weight, down_weight, nx, apart):
    width, ff = gate_weight.shape
    ny, _, _, cols = down_weight.shape
    rows = width // nx
    each = 2 + ny

    shapes = [(rows, 2 * ff + (0 if s in apart else cols)) for s in range(nx)] + [(rows, cols)] * len(apart)
    count = len(shapes)

    def kernel(at, gate, up, down, *refs):
        outs, held, sem, out_sem = refs[:count], refs[count : 2 * count], refs[2 * count], refs[2 * count + 1]
        order = list(range(1, nx)) + [0]
        loads = {}
        for s in order:
            quarter = lax.rem(at[0] + s, nx)
            down_at = (held[nx + apart.index(s)], 0) if s in apart else (held[s], 2 * ff)
            loads[s] = [
                pltpu.make_async_copy(
                    src.at[pl.ds(quarter * rows, rows)],
                    held[s].at[:, pl.ds(side * ff, ff)],
                    sem.at[each * s + side],
                )
                for side, src in enumerate((gate, up))
            ] + [
                pltpu.make_async_copy(
                    down.at[j, quarter],
                    down_at[0].at[pl.ds(j * ff, ff), pl.ds(down_at[1], cols)],
                    sem.at[each * s + 2 + j],
                )
                for j in range(ny)
            ]
            for copy in loads[s]:
                copy.start()
        stores = []
        for s in order:
            for copy in loads[s]:
                copy.wait()
            for i in [s] + ([nx + apart.index(s)] if s in apart else []):
                stores.append(pltpu.make_async_copy(held[i], outs[i], out_sem.at[i]))
                stores[-1].start()
        for copy in stores:
            copy.wait()

    return pl.pallas_call(
        kernel,
        out_shape=[jax.ShapeDtypeStruct(shape, BF16) for shape in shapes],
        in_specs=[SMEM, HBM, HBM, HBM],
        out_specs=[HBM] * count,
        scratch_shapes=[pltpu.VMEM(shape, BF16) for shape in shapes]
        + [pltpu.SemaphoreType.DMA((each * nx,)), pltpu.SemaphoreType.DMA((count,))],
        compiler_params=pltpu.CompilerParams(vmem_limit_bytes=WHOLE.vmem_limit_bytes - (512 << 10)),
        name="weight_quarters",
    )(x_at, gate_weight, up_weight, down_weight)


def dispatch(tp_at, tokens, ids, gain, experts, room, cols):
    rows, width = tokens.shape
    top = ids.shape[0]
    slots = experts * room
    chunks = 4 if rows % 64 == 0 else 1
    step = rows // chunks

    def kernel(at, tok_hbm, ids_hbm, gain_hbm, out, dest_ref, tok, ids_ref, gain_ref, own_ref, sem):
        start = pl.multiple_of(at[0] * cols, cols)
        small = [
            pltpu.make_async_copy(ids_hbm, ids_ref, sem.at[chunks]),
            pltpu.make_async_copy(gain_hbm.at[:, pl.ds(start, cols)], gain_ref, sem.at[chunks + 1]),
        ]
        large = [
            pltpu.make_async_copy(tok_hbm.at[pl.ds(i * step, step)], tok.at[pl.ds(i * step, step)], sem.at[i])
            for i in range(chunks)
        ]
        for copy in small + large:
            copy.start()
        for copy in small:
            copy.wait()
        expert = lax.broadcasted_iota(jnp.int32, (experts, rows), 0)
        here = [ids_ref[k : k + 1, :] == expert for k in range(top)]
        named = sum(h.astype(F32) for h in here).astype(BF16)
        earlier = lax.broadcasted_iota(jnp.int32, (rows, rows), 0) < lax.broadcasted_iota(
            jnp.int32, (rows, rows), 1
        )
        before = jnp.dot(named, earlier.astype(F32).astype(BF16), preferred_element_type=F32)
        slot = lax.broadcasted_iota(jnp.int32, (slots, rows), 0)
        pick = None
        for k in range(top):
            place = jnp.sum(jnp.where(here[k], before, 0.0), axis=0, keepdims=True).astype(jnp.int32)
            dest = ids_ref[k : k + 1, :] * room + place
            dest_ref[k : k + 1, :] = dest
            hit = (slot == dest).astype(F32)
            pick = hit if pick is None else pick + hit
        pick = pick.astype(BF16)
        for i in range(chunks):
            large[i].wait()
            at_rows = slice(i * step, (i + 1) * step)
            values = tok[at_rows, :].astype(F32)
            scale = lax.rsqrt(jnp.sum(values * values, axis=-1, keepdims=True) * (1.0 / width) + EPS)
            own = tok[at_rows, pl.ds(start, cols)].astype(F32)
            own_ref[at_rows, :] = (own * scale * gain_ref[...]).astype(BF16)
        out[...] = jnp.dot(pick, own_ref[...], preferred_element_type=F32).astype(BF16)

    return pl.pallas_call(
        kernel,
        out_shape=[jax.ShapeDtypeStruct((slots, cols), BF16), jax.ShapeDtypeStruct((top, rows), jnp.int32)],
        in_specs=[SMEM, HBM, HBM, HBM],
        out_specs=[VMEM, VMEM],
        scratch_shapes=[
            pltpu.VMEM((rows, width), BF16),
            pltpu.VMEM((top, rows), jnp.int32),
            pltpu.VMEM((1, cols), F32),
            pltpu.VMEM((rows, cols), BF16),
            pltpu.SemaphoreType.DMA((chunks + 2,)),
        ],
        compiler_params=WHOLE,
        name="dispatch",
    )(tp_at, tokens, ids, gain)


def used_slots(slots, rows, cap, room, slots_first):
    shape, at = ((slots, rows), 0) if slots_first else ((rows, slots), 1)
    slot = lax.broadcasted_iota(jnp.int32, shape, at)
    place = slot & (room - 1)
    row = lax.shift_right_logical(slot, room.bit_length() - 1) * cap + place
    hit = (row == lax.broadcasted_iota(jnp.int32, shape, 1 - at)) & (place < cap)
    return hit.astype(F32).astype(BF16)


def close_up(arrived, cap):
    nz, nc, room, cols = arrived.shape
    rows = nz * cap

    def kernel(x, out):
        pick = used_slots(nz * room, rows, cap, room, False)
        for c in range(nc):
            block = x[:, c].reshape(nz * room, cols)
            out[c * rows : (c + 1) * rows] = jnp.dot(pick, block, preferred_element_type=F32).astype(BF16)

    return pl.pallas_call(
        kernel,
        out_shape=jax.ShapeDtypeStruct((nc * rows, cols), BF16),
        in_specs=[VMEM],
        out_specs=VMEM,
        compiler_params=params(4),
        name="close_up",
    )(arrived)


def partial_products(x_at, left, weights, firsts, wide, groups):
    nx = len(weights)
    rows, depth = left.shape
    share = rows // groups
    pairs = 256 // wide

    def kernel(at, x, *refs):
        w, out = refs[:nx], refs[nx]
        for s in range(0, nx, pairs):
            right = [w[s + i][:, firsts[s + i] : firsts[s + i] + wide] for i in range(pairs)]
            right = right[0] if pairs == 1 else jnp.concatenate(right, axis=1)
            product = jnp.dot(x[...], right, preferred_element_type=F32).astype(BF16)
            for i in range(pairs):
                place = lax.rem(at[0] + (nx - s - i), nx)
                for g in range(groups):
                    out[g * nx + place] = product[g * share : (g + 1) * share, i * wide : (i + 1) * wide]

    return pl.pallas_call(
        kernel,
        out_shape=jax.ShapeDtypeStruct((groups * nx, share, wide), BF16),
        in_specs=[SMEM, VMEM] + [VMEM] * nx,
        out_specs=VMEM,
        compiler_params=params(16),
        cost_estimate=pl.CostEstimate(flops=2 * nx * rows * depth * wide, bytes_accessed=4 << 20, transcendentals=0),
        name="partial_products",
    )(x_at, left, *weights)


def hidden_units(parts):
    nx, rows, wide = parts.shape
    ff = wide // 2

    def kernel(p, out):
        total = p[0].astype(F32)
        for j in range(1, nx):
            total += p[j].astype(F32)
        gate = jnp.minimum(total[:, :ff], LIMIT)
        up_part = jnp.clip(total[:, ff:], -LIMIT, LIMIT)
        out[...] = ((up_part + 1.0) * gate * jax.nn.sigmoid(ALPHA * gate)).astype(BF16)

    return pl.pallas_call(
        kernel,
        out_shape=jax.ShapeDtypeStruct((rows, ff), BF16),
        in_specs=[VMEM],
        out_specs=VMEM,
        compiler_params=params(8),
        name="hidden_units",
    )(parts)


def from_neighbours(blocks, axis):
    n = lax.axis_size(axis)
    return {s: lax.ppermute(block, axis, shifted(n, s)) for s, block in blocks.items()}


def add_up(parts, groups, blocks, cap, room):
    total, rows, cols = parts.shape
    terms = total // groups

    def kernel(p, out):
        spread = used_slots(blocks * room, rows, cap, room, True)
        for g in range(groups):
            value = p[g * terms].astype(F32)
            for j in range(1, terms):
                value += p[g * terms + j].astype(F32)
            value = jnp.dot(spread, value.astype(BF16), preferred_element_type=F32).astype(BF16)
            out[:, g] = value.reshape(blocks, room, cols)

    return pl.pallas_call(
        kernel,
        out_shape=jax.ShapeDtypeStruct((blocks, groups, room, cols), BF16),
        in_specs=[VMEM],
        out_specs=VMEM,
        compiler_params=params(4),
        name="add_up",
    )(parts)


def combine(back, dest, route):
    slots, cols = back.shape
    top, rows = dest.shape

    def kernel(x, dest_ref, route_ref, out):
        slot = lax.broadcasted_iota(jnp.int32, (slots, rows), 0)
        same = lax.broadcasted_iota(jnp.int32, (rows, rows), 0) == lax.broadcasted_iota(jnp.int32, (rows, rows), 1)
        total = None
        for k in range(top):
            chosen = (slot == dest_ref[k : k + 1, :]).astype(F32).astype(BF16)
            copy = lax.dot_general(chosen, x[...], (((0,), (0,)), ((), ())), preferred_element_type=F32)
            weight = jnp.sum(jnp.where(same, route_ref[k : k + 1, :], 0.0), axis=1, keepdims=True)
            copy = copy * weight
            total = copy if total is None else total + copy
        out[...] = total.astype(BF16)

    return pl.pallas_call(
        kernel,
        out_shape=jax.ShapeDtypeStruct((rows, cols), BF16),
        in_specs=[VMEM, VMEM, VMEM],
        out_specs=VMEM,
        compiler_params=params(8),
        name="combine",
    )(back, dest, route)


def on_device(tokens, expert_ids, route_weight, norm_gain, gate_weight, up_weight, down_weight):
    nz, nc, ny, nx = (lax.axis_size(a) for a in ("z", "c", "y", "x"))
    x_at, y_at = lax.axis_index("x"), lax.axis_index("y")
    at = x_at.reshape(1).astype(jnp.int32)
    tp_at = (x_at * ny + y_at).reshape(1).astype(jnp.int32)
    rows, width = tokens.shape
    top = expert_ids.shape[1]
    experts = nz * nc * gate_weight.shape[0]
    cap = 5 * rows * top // (4 * experts)
    room = max(16, pl.next_power_of_2(cap))
    slots = experts * room
    cols = width // (nx * ny)
    ff = gate_weight.shape[2]

    buffer, dest = dispatch(tp_at, tokens, expert_ids.T, norm_gain.reshape(1, width), experts, room, cols)
    gate_weight, buffer = lax.optimization_barrier((gate_weight, buffer))
    apart = tuple(range(2, nx - 1))
    order = dict.fromkeys([1, nx - 1] + list(apart))
    weights = weight_quarters(
        at, gate_weight[0], up_weight[0], down_weight.reshape(ny, nx, ff, cols), nx, apart
    )

    arrived = swap(buffer.reshape(nz * nc, room, cols), ("z", "c")).reshape(nz, nc, room, cols)
    moved = {0: weights[0]} | from_neighbours({s: weights[s] for s in order}, "x")
    late = from_neighbours(dict(zip(apart, weights[nx:])), "x")
    first_weights = [moved[s] for s in range(nx)]
    second_weights = [late.get(s, moved[s]) for s in range(nx)]
    arrived = close_up(arrived, cap)
    left = lax.all_gather(arrived, "y", axis=1, tiled=True)
    parts = partial_products(at, left, first_weights, [0] * nx, 2 * ff, 1)
    parts = swap(parts, "x")

    hidden = lax.all_gather(hidden_units(parts), "y", axis=1, tiled=True)
    firsts = [0 if s in late else 2 * ff for s in range(nx)]
    parts = partial_products(at, hidden, second_weights, firsts, cols, nc)
    parts = swap(parts, ("c", "x"))

    result = add_up(parts, nc, nz, cap, room).reshape(nz, nc * room, cols)
    back = swap(result, "z").reshape(slots, cols)
    return combine(back, dest, route_weight.T)


def solution(mesh):
    torus = Mesh(mesh.devices.reshape(mesh.shape["ep"] // 2, 2, 8, 4), ("z", "c", "y", "x"))
    ep, tp = ("z", "c"), ("y", "x")
    in_specs = (
        P(ep, None),
        P(ep, None),
        P(ep, None),
        P(),
        P(ep, None, tp),
        P(ep, None, tp),
        P(ep, None, tp),
    )

    return jax.shard_map(on_device, mesh=torus, in_specs=in_specs, out_specs=P(ep, tp), check_vma=False)
```
